32 devices in a mesh: ep: 16 (over z, x, core), tp: 2 (over y).
Axes of the slice: x: 2, y: 2, z: 4, core: 2. Of those that a mesh axis runs over, the one named last changes fastest.
Arguments:
- tokens: bfloat16 [256, 1024], P('ep'), may hold values from -6 to 6
- old_state: float32 [256, 4, 128, 128], P('ep', 'tp'), may hold values from -6 to 6
- query_weight: bfloat16 [1024, 512], P(None, 'tp'), may hold values from -0.1875 to 0.1875
- forget_weight: bfloat16 [1024, 512], P(None, 'tp'), may hold values from -0.1875 to 0.1875
- input_weight: bfloat16 [1024, 512], P(None, 'tp'), may hold values from -0.1875 to 0.1875
- lower_bound: float32 [512], P('tp'), may hold values from 0 to 0.9
- head_gain: float32 [4, 128], P('tp'), may hold values from 0.1 to 1.9
- out_weight: bfloat16 [512, 1024], P('tp'), may hold values from -0.25 to 0.25
- mix_gain: float32 [1024], replicated, may hold values from 0.1 to 1.9
- ffn_gain: float32 [1024], replicated, may hold values from 0.1 to 1.9
- group_weight: bfloat16 [1024, 4], replicated, may hold values from -0.1875 to 0.1875
- expert_weight: bfloat16 [1024, 16], replicated, may hold values from -0.1875 to 0.1875
- routes: int32 [256, 6], P('ep'), may hold values from 0 to 15, all different within a row; in each aligned block of 16 rows (0 to 15, 16 to 31, ...) at most 12 rows name the same one
- gate_weight: bfloat16 [16, 1024, 1024], P('ep', None, 'tp'), may hold values from -0.1875 to 0.1875
- up_weight: bfloat16 [16, 1024, 1024], P('ep', None, 'tp'), may hold values from -0.1875 to 0.1875
- down_weight: bfloat16 [16, 1024, 1024], P('ep', None, 'tp'), may hold values from -0.1875 to 0.1875
Outputs:
- layer_out: bfloat16 [256, 1024], P('ep', 'tp')
- new_state: float32 [256, 4, 128, 128], P('ep', 'tp')
The draws below stay inside these ranges and needn't reach their ends.
Inputs may be any that keep to these rules, and one draw needn't show every extreme that they name: `routes`: each row names 6 different experts. In each aligned block of 16 rows (the rows of one device) no expert is named more than 12 times, a bound that some block reaches.
All inputs are finite; a program needn't handle non-finite values.
Results may differ from the reference program's by a relative error of at most 0.011.
Values may be sent and summed in bfloat16 or wider, within the bound.
A program may use at most 64 MiB of HBM per device.

```python
import math
import jax
import jax.numpy as jnp
import numpy as np
from jax import lax

D = 1024
HEADS = 4
HEAD_DIM = 128
FF = 1024
GROUPS = 4
TOPK = 6
SEQ_DEV = 16
HG = 512
EXPERTS = 16
CAP = 12
TOKENS = 256
N_EP = 16
N_TP = 2


def block_scale(stream_key, dims, pieces, smallest, largest):
    level, own = 1.0, jax.random.fold_in(stream_key, 6)
    for axis_at, parts in pieces:
        draws = jnp.exp(jax.random.uniform(jax.random.fold_in(own, axis_at), (parts,), jnp.float32, smallest / len(pieces), largest / len(pieces)))
        level = level * jnp.repeat(draws, dims[axis_at] // parts).reshape([-1 if axis == axis_at else 1 for axis in range(len(dims))])
    return level


def assign_block(rng, own, number, rows, amount, top, reach, skew):
    order = jax.random.permutation(rng, amount)
    crowded, common = shares(amount, rows * top, reach, skew, True), shares(amount, rows * top, reach, skew, False)
    places = jnp.arange(amount)

    def named(lengths, offset_by):
        used = int((lengths > 0).sum())
        fixed = max(1, used // 4)
        moved = fixed + (places - fixed + offset_by * (used - fixed)) % max(1, amount - fixed)
        return jnp.zeros((amount,), jnp.int32).at[order[jnp.where(places < fixed, places, moved)]].set(jnp.asarray(lengths, jnp.int32))

    lengths = jnp.where(number % 4 == 0, named(crowded, number // 4), named(common, number - number // 4 - 1))
    mixed = jax.random.permutation(jax.random.fold_in(own, 3), amount)
    source_of, receiver = mixed[0:amount // 2 * 2:2], mixed[1:amount // 2 * 2:2]
    margin = jnp.minimum(lengths[source_of] - 1, reach - lengths[receiver]) // 2
    margin = jnp.where((source_of == order[0]) | (receiver == order[0]) | (lengths[receiver] == 0), 0, jnp.maximum(margin, 0))
    moved = jax.random.randint(jax.random.fold_in(own, 4), (amount // 2,), 0, 1 << 20) % (margin + 1)
    lengths = lengths.at[source_of].add(-moved).at[receiver].add(moved)
    members = jnp.searchsorted(jnp.cumsum(lengths), jnp.arange(rows * top), side="right").astype(jnp.int32)
    table = members.reshape(top, rows).T
    table = table[jax.random.permutation(jax.random.fold_in(own, 1), rows)]
    offset_by = jax.random.randint(jax.random.fold_in(own, 2), (rows, 1), 0, top)
    return jnp.take_along_axis(table, (jnp.arange(top)[None, :] + offset_by) % top, axis=1)


def shares(number_of, total, bound, skew, full):
    portions = [(1 << 20) // math.isqrt(standing ** skew) + 1 for standing in range(1, number_of + 1)]
    largest = bound if full else min(bound, max(-(-total // number_of), total * portions[0] // sum(portions)))
    least = 1 if total - largest >= number_of - 1 else 0
    given, rest = [largest] + [least] * (number_of - 1), total - largest - least * (number_of - 1)
    while rest > 0:
        candidates = [i for i in range(1, number_of) if given[i] < largest] or [i for i in range(1, number_of) if given[i] < bound]
        whole, left = sum([portions[i] for i in candidates]), rest
        for i in candidates:
            more = min(bound - given[i], max(1, left * portions[i] // whole), rest)
            given[i] = given[i] + more
            rest = rest - more
    return np.array(given)


def gaussian(stream_key, shape, width, most, pieces=(), kind=jnp.bfloat16):
    level = block_scale(stream_key, shape, pieces, -0.22, 0.18) if pieces else 1.0
    values = jax.random.normal(stream_key, shape, jnp.float32) * width * level
    return jnp.minimum(jnp.maximum(values, -most), most).astype(kind)


def setup_inputs(seed: int = 0) -> dict:
    splits = jax.random.split(jax.random.key(seed), 17)
    tokens = gaussian(splits[0], (TOKENS, D), 1.0, 6.0, ((0, 16),))
    old_state = gaussian(splits[1], (TOKENS, HEADS, HEAD_DIM, HEAD_DIM), 1.0, 6.0, ((0, 16), (1, 2)), jnp.float32)
    query_weight = gaussian(splits[2], (D, HG), D ** -0.5, 0.1875, ((1, 2),))
    forget_weight = gaussian(splits[3], (D, HG), D ** -0.5, 0.1875, ((1, 2),))
    input_weight = gaussian(splits[4], (D, HG), D ** -0.5, 0.1875, ((1, 2),))
    lower_bound = jnp.clip(0.9 * jax.random.uniform(splits[5], (HG,), jnp.float32) ** block_scale(splits[5], (HG,), ((0, 2),), -0.2, 0.2), 0.0, 0.9)
    head_gain = jnp.clip(1.0 + 0.18 * jax.random.normal(splits[6], (HEADS, HEAD_DIM), jnp.float32), 0.1, 1.9)
    out_weight = gaussian(splits[7], (HG, D), HG ** -0.5, 0.25, ((0, 2),))
    mix_gain = jnp.clip(1.0 + 0.18 * jax.random.normal(splits[8], (D,), jnp.float32), 0.1, 1.9)
    ffn_gain = jnp.clip(1.0 + 0.18 * jax.random.normal(splits[9], (D,), jnp.float32), 0.1, 1.9)
    group_weight = gaussian(splits[10], (D, GROUPS), D ** -0.5, 0.1875)
    expert_weight = gaussian(splits[11], (D, EXPERTS), D ** -0.5, 0.1875)
    routes_keys = jax.random.split(jax.random.fold_in(splits[12], 1), TOKENS // SEQ_DEV)
    routes_turns = jax.random.permutation(jax.random.fold_in(splits[12], 3), TOKENS // SEQ_DEV)
    routes = jax.vmap(lambda own, number: assign_block(jax.random.fold_in(splits[12], 2), own, number, SEQ_DEV, EXPERTS, TOPK, CAP, 2))(routes_keys, routes_turns).reshape((TOKENS, TOPK))
    gate_weight = gaussian(splits[13], (EXPERTS, D, FF), D ** -0.5, 0.1875, ((0, 16), (2, 2)))
    up_weight = gaussian(splits[14], (EXPERTS, D, FF), D ** -0.5, 0.1875, ((0, 16), (2, 2)))
    down_weight = gaussian(splits[15], (EXPERTS, FF, D), FF ** -0.5, 0.1875, ((0, 16), (2, 2)))
    return {"tokens": tokens, "old_state": old_state, "query_weight": query_weight, "forget_weight": forget_weight, "input_weight": input_weight, "lower_bound": lower_bound, "head_gain": head_gain, "out_weight": out_weight, "mix_gain": mix_gain, "ffn_gain": ffn_gain, "group_weight": group_weight, "expert_weight": expert_weight, "routes": routes, "gate_weight": gate_weight, "up_weight": up_weight, "down_weight": down_weight}


epsilon = 1e-06

def scaled_rms(values, gain):
    return values * lax.rsqrt(lax.optimization_barrier(jnp.mean(values * values, axis=-1, keepdims=True)) + epsilon) * gain

def block_slots(route_blocks):
    hits = (route_blocks[:, :, None] == jnp.arange(EXPERTS, dtype=jnp.int32)[None, None, :]).astype(jnp.int32)
    before = jnp.cumsum(hits, axis=1) - hits
    return lax.optimization_barrier(jnp.sum(hits * before, axis=2))

def reference(tokens, old_state, query_weight, forget_weight, input_weight, lower_bound, head_gain, out_weight, mix_gain, ffn_gain, group_weight, expert_weight, routes, gate_weight, up_weight, down_weight):
    resident = tokens.astype(jnp.float32)
    normed = scaled_rms(resident, mix_gain).astype(jnp.bfloat16)
    query_pre = jnp.dot(normed, query_weight, preferred_element_type=jnp.float32)
    forget_pre = jnp.dot(normed, forget_weight, preferred_element_type=jnp.float32)
    input_pre = jnp.dot(normed, input_weight, preferred_element_type=jnp.float32)
    query = jax.nn.silu(query_pre).reshape(TOKENS, HEADS, HEAD_DIM)
    forget = (lower_bound + (1.0 - lower_bound) * jax.nn.sigmoid(forget_pre)).reshape(TOKENS, HEADS, HEAD_DIM)
    value = input_pre.reshape(TOKENS, HEADS, HEAD_DIM)
    new_state = forget[..., None] * old_state + (1.0 - forget)[..., None] * value[:, :, None, :]
    readout = lax.optimization_barrier(jnp.sum(new_state * query[..., None], axis=2))
    head_out = scaled_rms(readout, head_gain).astype(jnp.bfloat16).reshape(TOKENS, HEADS * HEAD_DIM)
    width_block = HEADS * HEAD_DIM // N_TP
    mixed = jnp.zeros((TOKENS, D), jnp.float32)
    for index in range(N_TP):
        lower = index * width_block
        partial_sum = jnp.dot(head_out[:, lower:lower + width_block], out_weight[lower:lower + width_block], preferred_element_type=jnp.float32)
        rounded = lax.optimization_barrier(partial_sum.astype(jnp.bfloat16))
        mixed = mixed + rounded.astype(jnp.float32)
    mixed_rounded = lax.optimization_barrier(mixed.astype(jnp.bfloat16))
    residual = (resident + mixed_rounded.astype(jnp.float32)).astype(jnp.bfloat16)
    ffn_in = scaled_rms(residual.astype(jnp.float32), ffn_gain).astype(jnp.bfloat16)
    group_raw = jnp.exp(jnp.dot(ffn_in, group_weight, preferred_element_type=jnp.float32))
    group_prob = group_raw / lax.optimization_barrier(jnp.sum(group_raw, axis=-1, keepdims=True))
    per_group = EXPERTS // GROUPS
    expert_raw = jnp.exp(jnp.dot(ffn_in, expert_weight, preferred_element_type=jnp.float32)).reshape(TOKENS, GROUPS, per_group)
    expert_prob = expert_raw / lax.optimization_barrier(jnp.sum(expert_raw, axis=-1, keepdims=True)) * group_prob[:, :, None]
    expert_prob = expert_prob.reshape(TOKENS, EXPERTS)
    chosen = routes[:, :, None] == jnp.arange(EXPERTS, dtype=jnp.int32)[None, None, :]
    weight = lax.optimization_barrier(jnp.sum(jnp.where(chosen, expert_prob[:, None, :], 0.0), axis=-1))
    gate = weight / lax.optimization_barrier(jnp.sum(weight, axis=-1, keepdims=True))
    rows_per = N_EP * CAP
    slots = block_slots(routes.reshape(N_EP, SEQ_DEV * TOPK)).reshape(-1)
    flat = routes.reshape(-1)
    owner = jnp.arange(TOKENS * TOPK, dtype=jnp.int32) // (SEQ_DEV * TOPK)
    target = (flat * rows_per + owner * CAP + slots).astype(jnp.int32)
    token_of = jnp.arange(TOKENS * TOPK, dtype=jnp.int32) // TOPK
    buffer = jnp.zeros((EXPERTS * rows_per, D), jnp.bfloat16).at[target].set(ffn_in[token_of])
    buffer = buffer.reshape(EXPERTS, rows_per, D)

    def expert(inputs):
        rows, gate_part, up_part, down_part = inputs
        hidden = (jax.nn.silu(jnp.dot(rows, gate_part, preferred_element_type=jnp.float32)) * jnp.dot(rows, up_part, preferred_element_type=jnp.float32)).astype(jnp.bfloat16)
        return jnp.dot(hidden, down_part, preferred_element_type=jnp.float32).astype(jnp.bfloat16)
    produced = lax.map(expert, (buffer, gate_weight, up_weight, down_weight)).reshape(EXPERTS * rows_per, D)
    picked = produced[target].astype(jnp.float32).reshape(TOKENS, TOPK, D)
    mixture = lax.optimization_barrier(jnp.sum(gate[:, :, None] * picked, axis=1))
    layer_out = (residual.astype(jnp.float32) + mixture).astype(jnp.bfloat16)
    return (layer_out, new_state)
```

```python
import functools

import jax
import jax.numpy as jnp
from jax import lax
from jax.experimental import pallas as pl
from jax.experimental.pallas import tpu as pltpu
from jax.sharding import PartitionSpec as P

epsilon = 1e-06
MESH = pl.DeviceIdType.MESH
BF16 = jnp.bfloat16
F32 = jnp.float32


def scaled_rms(values, gain):
    return values * lax.rsqrt(jnp.mean(values * values, axis=-1, keepdims=True) + epsilon) * gain


def dot(a, b):
    return jnp.dot(a, b, preferred_element_type=F32)


def other(index, step, count):
    total, bit = 0, 1
    while bit < count:
        total = total + ((index // bit + (step // bit) % 2) % 2) * bit
        bit *= 2
    return total


def mix_kernel(
    tokens, gain, lower, head_gain, qw, fw, iw, ow, state, new_state, part,
    wq, wf, wi, wo, st, readout, w_sem, in_sem, out_sem, chunks,
):
    seq, heads, size = st.shape[0], st.shape[1], st.shape[2]
    loads = [
        pltpu.make_async_copy(src, dst, w_sem.at[k])
        for k, (src, dst) in enumerate(((fw, wf), (iw, wi), (qw, wq)))
    ]
    for copy in loads:
        copy.start()
    step = seq // chunks
    ins, outs = [], []
    for k in range(chunks):
        rows = pl.ds(k * step, step)
        ins.append(pltpu.make_async_copy(state.at[rows], st.at[rows], in_sem.at[k]))
        outs.append(pltpu.make_async_copy(st.at[rows], new_state.at[rows], out_sem.at[k]))
        ins[k].start()
    out_load = pltpu.make_async_copy(ow, wo, w_sem.at[3])
    out_load.start()
    normed = scaled_rms(tokens[...].astype(F32), gain[...]).astype(BF16)
    loads[0].wait()
    forget_pre = dot(normed, wf[...])
    low = lower[...]
    forget = low + (1.0 - low) * (1.0 / (1.0 + jnp.exp(-forget_pre)))
    forget_t = forget.T
    loads[1].wait()
    value = dot(normed, wi[...])
    loads[2].wait()
    query_pre = dot(normed, wq[...])
    query = query_pre / (1.0 + jnp.exp(-query_pre))
    query_t = query.T
    for k in range(chunks):
        ins[k].wait()
        for t in range(k * step, (k + 1) * step):
            for h in range(heads):
                cols = slice(h * size, (h + 1) * size)
                f = forget_t[cols, t : t + 1]
                q = query_t[cols, t : t + 1]
                v = value[t : t + 1, cols]
                fresh = f * st[t, h] + (1.0 - f) * v
                st[t, h] = fresh
                readout[h, t : t + 1, :] = jnp.sum(fresh * q, axis=0, keepdims=True)
        outs[k].start()
    out_load.wait()
    total = None
    for h in range(heads):
        head_out = scaled_rms(readout[h], head_gain[h : h + 1, :]).astype(BF16)
        term = dot(head_out, wo[h * size : (h + 1) * size, :])
        total = term if total is None else total + term
    part[...] = total.astype(BF16)
    for k in range(chunks):
        outs[k].wait()


def expert_kernel(
    dims, tokens, part, gain, group_t, expert_t, routes, gw, uw, dw, out,
    wg, wu, wd, parts, resid, x, hid, y, p, q, qr, u, v,
    w_sem, a_s, a_r, z_s, z_r, x_s, x_r, d_s, d_r, h_s, h_r,
    b_s, b_r, c_s, c_r, e_s, e_r,
):
    Z, C, X, TP = dims
    seq, width = tokens.shape
    ep, tp = lax.axis_index("ep"), lax.axis_index("tp")
    core, col, row = ep % C, (ep // C) % X, ep // (C * X)
    cols = out.shape[1]
    experts = expert_t.shape[0]
    groups = group_t.shape[0]

    def ep_of(a, b, c):
        return (a * X + b) * C + c

    z_peers = [other(row, s, Z) for s in range(Z)]
    x_peers = [other(col, d, X) for d in range(X)]
    t_peers = [other(tp, d, TP) for d in range(TP)]
    mate = ep_of(row, col, 1 - core)

    barrier = pltpu.get_barrier_semaphore()
    greet = [{"ep": ep_of(a, col, core)} for a in z_peers[1:]]
    greet += [{"ep": ep_of(row, b, core)} for b in x_peers[1:]]
    greet += [{"tp": t} for t in t_peers[1:]] + [{"ep": mate}]
    for who in greet:
        pl.semaphore_signal(barrier, inc=1, device_id=who, device_id_type=MESH)
    loads = [
        pltpu.make_async_copy(src.at[0], dst, w_sem.at[k])
        for k, (src, dst) in enumerate(((gw, wg), (uw, wu), (dw, wd)))
    ]
    for copy in loads:
        copy.start()
    pl.semaphore_wait(barrier, len(greet))

    started = []

    def send(src, dst, s_sem, r_sem, who):
        copy = pltpu.make_async_remote_copy(
            src_ref=src, dst_ref=dst, send_sem=s_sem, recv_sem=r_sem,
            device_id=who, device_id_type=MESH,
        )
        copy.start()
        started.append(copy)
        return copy

    first = [
        send(part, parts.at[tp], a_s.at[d], a_r.at[d], {"tp": t_peers[d]}) for d in range(1, TP)
    ]
    parts[tp] = part[...]
    for copy in first:
        copy.wait_recv()
    mixed = parts[0].astype(F32)
    for j in range(1, TP):
        mixed = mixed + parts[j].astype(F32)
    mixed = mixed.astype(BF16).astype(F32)
    residual = (tokens[...].astype(F32) + mixed).astype(BF16).astype(F32)
    resid[...] = residual
    ffn_in = scaled_rms(residual, gain[...]).astype(BF16)

    contract = (((1,), (1,)), ((), ()))
    group_raw = jnp.exp(
        lax.dot_general(ffn_in, group_t[...], contract, preferred_element_type=F32)
    )
    group_sum = jnp.sum(group_raw, axis=-1, keepdims=True)
    expert_raw = jnp.exp(
        lax.dot_general(ffn_in, expert_t[...], contract, preferred_element_type=F32)
    )
    lane = lax.broadcasted_iota(jnp.int32, (seq, experts), 1)
    per = experts // groups
    prob = jnp.zeros((seq, experts), F32)
    for g in range(groups):
        member = (lane >= g * per) & (lane < (g + 1) * per)
        total = jnp.sum(jnp.where(member, expert_raw, 0.0), axis=-1, keepdims=True)
        share = group_raw[:, g : g + 1] / group_sum
        prob = jnp.where(member, expert_raw / total * share, prob)
    chosen = lane < 0
    for k in range(routes.shape[1]):
        chosen = chosen | (routes[:, k : k + 1] == lane)
    weight = jnp.where(chosen, prob, 0.0)
    gate = weight / jnp.sum(weight, axis=-1, keepdims=True)
    gate_hi = gate.astype(BF16)
    gate_lo = (gate - gate_hi.astype(F32)).astype(BF16)
    extra = x.shape[-1] - width
    tail = [gate_hi.astype(F32), gate_lo.astype(F32)]
    if extra > 2 * experts:
        tail.append(jnp.zeros((seq, extra - 2 * experts), F32))
    x[row, core, col, :, :width] = ffn_in
    x[row, core, col, :, width:] = jnp.concatenate(tail, axis=1).astype(BF16)

    mine = x.at[row, core, col]
    to_z = [None] + [
        send(mine, mine, z_s.at[s], z_r.at[s], {"ep": ep_of(z_peers[s], col, core)})
        for s in range(1, Z)
    ]

    def send_x(s):
        block = x.at[z_peers[s], core, col]
        return [
            send(block, block, x_s.at[s, d], x_r.at[s, d], {"ep": ep_of(row, x_peers[d], core)})
            for d in range(1, X)
        ]

    def send_d(s):
        column = x.at[z_peers[s], core]
        return send(column, column, d_s.at[s], d_r.at[s], {"ep": mate})

    to_x, to_d = [send_x(0)], []

    def pass_on(s):
        for copy in to_x[s]:
            copy.wait_recv()
        to_d.append(send_d(s))

    rows = C * X * seq
    to_h = []

    def expand(s):
        to_d[s].wait_recv()
        block = x[z_peers[s], :, :, :, :width].reshape(rows, width)
        g = dot(block, wg[...])
        up = dot(block, wu[...])
        hid[z_peers[s], tp] = (g / (1.0 + jnp.exp(-g)) * up).astype(BF16)
        piece = hid.at[z_peers[s], tp]
        to_h.append(
            [
                send(piece, piece, h_s.at[s, d], h_r.at[s, d], {"tp": t_peers[d]})
                for d in range(1, TP)
            ]
        )

    for s in range(1, Z):
        if s == 1:
            pass_on(0)
        to_z[s].wait_recv()
        to_x.append(send_x(s))
    if Z == 1:
        pass_on(0)
    loads[0].wait()
    loads[1].wait()
    for s in range(Z):
        if s + 1 < Z:
            pass_on(s + 1)
        expand(s)
    loads[2].wait()

    to_b, to_c, to_e = {}, {}, {}
    half = wd.shape[0] // TP

    def contract_rows(s):
        for copy in to_h[s]:
            copy.wait_recv()
        total = None
        for j in range(TP):
            term = dot(hid[z_peers[s], j], wd[j * half : (j + 1) * half, :])
            total = term if total is None else total + term
        tags = x[z_peers[s], :, :, :, width:].reshape(rows, extra).astype(F32)
        at = lax.broadcasted_iota(jnp.int32, (rows, extra), 1)
        own = (at == ep) | (at == ep + experts)
        scale = jnp.sum(jnp.where(own, tags, 0.0), axis=-1, keepdims=True)
        y[s] = (total * scale).astype(BF16).reshape(C, X, seq, cols)
        to_b[s] = send(y.at[s, 1 - core], p.at[s], b_s.at[s], b_r.at[s], {"ep": mate})

    def join_cores(s):
        to_b[s].wait_recv()
        q[s] = (y[s, core].astype(F32) + p[s].astype(F32)).astype(BF16)
        to_c[s] = [
            send(
                q.at[s, x_peers[d]], qr.at[s, d], c_s.at[s, d], c_r.at[s, d],
                {"ep": ep_of(row, x_peers[d], core)},
            )
            for d in range(1, X)
        ]

    def join_columns(s):
        total = q[s, col].astype(F32)
        for d in range(1, X):
            to_c[s][d - 1].wait_recv()
            total = total + qr[s, d].astype(F32)
        if s == 0:
            return total
        u[s] = total.astype(BF16)
        to_e[s] = send(
            u.at[s], v.at[s], e_s.at[s], e_r.at[s], {"ep": ep_of(z_peers[s], col, core)}
        )

    order = list(range(Z))[::-1]
    order = list(range(1, Z)) + [0]
    result = None
    for k in range(Z + 2):
        if k < Z:
            contract_rows(order[k])
        if 1 <= k < Z + 1:
            join_cores(order[k - 1])
        if k >= 2:
            result = join_columns(order[k - 2])
    for s in range(1, Z):
        to_e[s].wait_recv()
        result = result + v[s].astype(F32)
    own_resid = resid[:, pl.ds(pl.multiple_of(tp * cols, cols), cols)]
    out[...] = (own_resid + result).astype(BF16)
    for copy in started:
        copy.wait_send()


def local(
    dims,
    tokens,
    old_state,
    query_weight,
    forget_weight,
    input_weight,
    lower_bound,
    head_gain,
    out_weight,
    mix_gain,
    ffn_gain,
    group_weight,
    expert_weight,
    routes,
    gate_weight,
    up_weight,
    down_weight,
):
    Z, C, X, TP = dims
    seq, width = tokens.shape
    heads, size = old_state.shape[1], old_state.shape[2]
    experts = expert_weight.shape[1]
    channels = query_weight.shape[1]
    hidden, cols = gate_weight.shape[2], down_weight.shape[2]
    vmem = pl.BlockSpec(memory_space=pltpu.VMEM)
    anywhere = pl.BlockSpec(memory_space=pl.ANY)
    chunks = 4 if seq % 4 == 0 else 1
    dma = pltpu.SemaphoreType.DMA
    new_state, part = pl.pallas_call(
        functools.partial(mix_kernel, chunks=chunks),
        out_shape=(
            jax.ShapeDtypeStruct(old_state.shape, F32),
            jax.ShapeDtypeStruct((seq, width), BF16),
        ),
        in_specs=[vmem] * 4 + [anywhere] * 5,
        out_specs=(anywhere, vmem),
        scratch_shapes=[
            pltpu.VMEM((width, channels), BF16),
            pltpu.VMEM((width, channels), BF16),
            pltpu.VMEM((width, channels), BF16),
            pltpu.VMEM((channels, width), BF16),
            pltpu.VMEM(old_state.shape, F32),
            pltpu.VMEM((heads, seq, size), F32),
            dma((4,)),
            dma((chunks,)),
            dma((chunks,)),
        ],
        name="mix",
    )(
        tokens, mix_gain[None], lower_bound[None], head_gain,
        query_weight, forget_weight, input_weight, out_weight, old_state,
    )
    extra = -(-2 * experts // 128) * 128
    block = (seq, width + extra)
    layer_out = pl.pallas_call(
        functools.partial(expert_kernel, dims),
        out_shape=jax.ShapeDtypeStruct((seq, cols), BF16),
        in_specs=[vmem] * 6 + [anywhere] * 3,
        out_specs=vmem,
        scratch_shapes=[
            pltpu.VMEM((width, hidden), BF16),
            pltpu.VMEM((width, hidden), BF16),
            pltpu.VMEM((hidden * TP, cols), BF16),
            pltpu.VMEM((TP, seq, width), BF16),
            pltpu.VMEM((seq, width), F32),
            pltpu.VMEM((Z, C, X) + block, BF16),
            pltpu.VMEM((Z, TP, C * X * seq, hidden), BF16),
            pltpu.VMEM((Z, C, X, seq, cols), BF16),
            pltpu.VMEM((Z, X, seq, cols), BF16),
            pltpu.VMEM((Z, X, seq, cols), BF16),
            pltpu.VMEM((Z, X, seq, cols), BF16),
            pltpu.VMEM((Z, seq, cols), BF16),
            pltpu.VMEM((Z, seq, cols), BF16),
            dma((3,)),
            dma((TP,)), dma((TP,)),
            dma((Z,)), dma((Z,)),
            dma((Z, X)), dma((Z, X)),
            dma((Z,)), dma((Z,)),
            dma((Z, TP)), dma((Z, TP)),
            dma((Z,)), dma((Z,)),
            dma((Z, X)), dma((Z, X)),
            dma((Z,)), dma((Z,)),
        ],
        compiler_params=pltpu.CompilerParams(collective_id=0, has_side_effects=True),
        name="experts",
    )(
        tokens, part, ffn_gain[None], group_weight.T, expert_weight.T, routes,
        gate_weight, up_weight, down_weight,
    )
    return (layer_out, new_state)


def solution(mesh):
    in_specs = (
        P("ep", None),
        P("ep", "tp", None, None),
        P(None, "tp"),
        P(None, "tp"),
        P(None, "tp"),
        P("tp"),
        P("tp", None),
        P("tp", None),
        P(),
        P(),
        P(),
        P(),
        P("ep", None),
        P("ep", None, "tp"),
        P("ep", None, "tp"),
        P("ep", None, "tp"),
    )
    out_specs = (P("ep", "tp"), P("ep", "tp", None, None))
    ep, tp = mesh.shape["ep"], mesh.shape["tp"]
    cores = 2
    across = tp
    dims = (ep // (cores * across), cores, across, tp)
    body = functools.partial(local, dims)
    return jax.shard_map(body, mesh=mesh, in_specs=in_specs, out_specs=out_specs, check_vma=False)
```

```python
import functools

import jax
import jax.numpy as jnp
from jax import lax
from jax.experimental import pallas as pl
from jax.experimental.pallas import tpu as pltpu
from jax.sharding import PartitionSpec as P

epsilon = 1e-06
MESH = pl.DeviceIdType.MESH
BF16 = jnp.bfloat16
F32 = jnp.float32


def scaled_rms(values, gain):
    return values * lax.rsqrt(jnp.mean(values * values, axis=-1, keepdims=True) + epsilon) * gain


def dot(a, b):
    return jnp.dot(a, b, preferred_element_type=F32)


def other(index, step, count):
    total, bit = 0, 1
    while bit < count:
        total = total + ((index // bit + (step // bit) % 2) % 2) * bit
        bit *= 2
    return total


def mix_kernel(
    tokens, gain, lower, head_gain, qw, fw, iw, ow, state, new_state, part,
    wq, wf, wi, wo, st, readout, w_sem, in_sem, out_sem, chunks,
):
    seq, heads, size = st.shape[0], st.shape[1], st.shape[2]
    loads = [
        pltpu.make_async_copy(src, dst, w_sem.at[k])
        for k, (src, dst) in enumerate(((fw, wf), (iw, wi), (qw, wq)))
    ]
    for copy in loads:
        copy.start()
    step = seq // chunks
    ins, outs = [], []
    for k in range(chunks):
        rows = pl.ds(k * step, step)
        ins.append(pltpu.make_async_copy(state.at[rows], st.at[rows], in_sem.at[k]))
        outs.append(pltpu.make_async_copy(st.at[rows], new_state.at[rows], out_sem.at[k]))
        ins[k].start()
    out_load = pltpu.make_async_copy(ow, wo, w_sem.at[3])
    out_load.start()
    normed = scaled_rms(tokens[...].astype(F32), gain[...]).astype(BF16)
    loads[0].wait()
    forget_pre = dot(normed, wf[...])
    low = lower[...]
    forget = low + (1.0 - low) * (1.0 / (1.0 + jnp.exp(-forget_pre)))
    forget_t = forget.T
    loads[1].wait()
    value = dot(normed, wi[...])
    loads[2].wait()
    query_pre = dot(normed, wq[...])
    query = query_pre / (1.0 + jnp.exp(-query_pre))
    query_t = query.T
    for k in range(chunks):
        ins[k].wait()
        for t in range(k * step, (k + 1) * step):
            for h in range(heads):
                cols = slice(h * size, (h + 1) * size)
                f = forget_t[cols, t : t + 1]
                q = query_t[cols, t : t + 1]
                v = value[t : t + 1, cols]
                fresh = f * st[t, h] + (1.0 - f) * v
                st[t, h] = fresh
                readout[h, t : t + 1, :] = jnp.sum(fresh * q, axis=0, keepdims=True)
        outs[k].start()
    out_load.wait()
    total = None
    for h in range(heads):
        head_out = scaled_rms(readout[h], head_gain[h : h + 1, :]).astype(BF16)
        term = dot(head_out, wo[h * size : (h + 1) * size, :])
        total = term if total is None else total + term
    part[...] = total.astype(BF16)
    for k in range(chunks):
        outs[k].wait()


def expert_kernel(
    dims, tokens, part, gain, group_t, expert_t, routes_t, gw, uw, dw, out,
    wg, wu, wd, parts, resid, x, hid, y, p, u, v,
    w_sem, a_s, a_r, z_s, z_r, x_s, x_r, d_s, d_r, h_s, h_r,
    b_s, b_r, e_s, e_r,
):
    Z, C, X, TP = dims
    seq, width = tokens.shape
    ep, tp = lax.axis_index("ep"), lax.axis_index("tp")
    core, col, row = ep % C, (ep // C) % X, ep // (C * X)
    cols = out.shape[1]
    experts = expert_t.shape[0]
    groups = group_t.shape[0]

    def ep_of(a, b, c):
        return (a * X + b) * C + c

    z_peers = [other(row, s, Z) for s in range(Z)]
    x_peers = [other(col, d, X) for d in range(X)]
    t_peers = [other(tp, d, TP) for d in range(TP)]
    c_peers = [other(core, d, C) for d in range(C)]
    mate = ep_of(row, col, c_peers[1])

    barrier = pltpu.get_barrier_semaphore()
    greet = [{"ep": ep_of(a, col, core)} for a in z_peers[1:]]
    greet += [{"ep": ep_of(row, b, c)} for b in x_peers[1:] for c in c_peers]
    greet += [{"tp": t} for t in t_peers[1:]] + [{"ep": mate}]
    for who in greet:
        pl.semaphore_signal(barrier, inc=1, device_id=who, device_id_type=MESH)
    loads = [
        pltpu.make_async_copy(src.at[0], dst, w_sem.at[k])
        for k, (src, dst) in enumerate(((gw, wg), (uw, wu), (dw, wd)))
    ]
    for copy in loads:
        copy.start()
    pl.semaphore_wait(barrier, len(greet))

    started = []

    def send(src, dst, s_sem, r_sem, who):
        copy = pltpu.make_async_remote_copy(
            src_ref=src, dst_ref=dst, send_sem=s_sem, recv_sem=r_sem,
            device_id=who, device_id_type=MESH,
        )
        copy.start()
        started.append(copy)
        return copy

    first = [
        send(part, parts.at[tp], a_s.at[d], a_r.at[d], {"tp": t_peers[d]}) for d in range(1, TP)
    ]
    parts[tp] = part[...]
    for copy in first:
        copy.wait_recv()
    mixed = parts[0].astype(F32)
    for j in range(1, TP):
        mixed = mixed + parts[j].astype(F32)
    mixed = mixed.astype(BF16).astype(F32)
    residual = (tokens[...].astype(F32) + mixed).astype(BF16).astype(F32)
    resid[...] = residual
    ffn_in = scaled_rms(residual, gain[...]).astype(BF16)

    contract = (((1,), (1,)), ((), ()))
    group_raw = jnp.exp(
        lax.dot_general(ffn_in, group_t[...], contract, preferred_element_type=F32)
    )
    group_sum = jnp.sum(group_raw, axis=-1, keepdims=True)
    expert_raw = jnp.exp(
        lax.dot_general(ffn_in, expert_t[...], contract, preferred_element_type=F32)
    )
    lane = lax.broadcasted_iota(jnp.int32, (seq, experts), 1)
    per = experts // groups
    prob = jnp.zeros((seq, experts), F32)
    for g in range(groups):
        member = (lane >= g * per) & (lane < (g + 1) * per)
        total = jnp.sum(jnp.where(member, expert_raw, 0.0), axis=-1, keepdims=True)
        share = group_raw[:, g : g + 1] / group_sum
        prob = jnp.where(member, expert_raw / total * share, prob)
    named = routes_t[...].astype(F32).T.astype(jnp.int32)
    chosen = lane < 0
    for k in range(routes_t.shape[0]):
        chosen = chosen | (named[:, k : k + 1] == lane)
    weight = jnp.where(chosen, prob, 0.0)
    gate = weight / jnp.sum(weight, axis=-1, keepdims=True)
    gate_hi = gate.astype(BF16)
    gate_lo = (gate - gate_hi.astype(F32)).astype(BF16)
    extra = x.shape[-1] - width
    tail = [gate_hi.astype(F32), gate_lo.astype(F32)]
    if extra > 2 * experts:
        tail.append(jnp.zeros((seq, extra - 2 * experts), F32))
    x[row, core, col, :, :width] = ffn_in
    x[row, core, col, :, width:] = jnp.concatenate(tail, axis=1).astype(BF16)

    mine = x.at[row, core, col]
    far_first = list(range(1, Z))[::-1]
    to_z = {
        s: send(mine, mine, z_s.at[s], z_r.at[s], {"ep": ep_of(z_peers[s], col, core)})
        for s in far_first
    }

    def send_x(s):
        block = x.at[z_peers[s], core, col]
        return [
            send(block, block, x_s.at[s, d], x_r.at[s, d], {"ep": ep_of(row, x_peers[d], core)})
            for d in range(1, X)
        ]

    def send_d(s):
        column = x.at[z_peers[s], core]
        return send(column, column, d_s.at[s], d_r.at[s], {"ep": mate})

    to_x, to_d = {0: send_x(0)}, {}

    def pass_on(s):
        for copy in to_x[s]:
            copy.wait_recv()
        to_d[s] = send_d(s)

    rows = C * X * seq
    to_h = {}

    def expand(s):
        to_d[s].wait_recv()
        block = x[z_peers[s], :, :, :, :width].reshape(rows, width)
        g = dot(block, wg[...])
        up = dot(block, wu[...])
        hid[z_peers[s], tp] = (g / (1.0 + jnp.exp(-g)) * up).astype(BF16)
        piece = hid.at[z_peers[s], tp]
        to_h[s] = [
            send(piece, piece, h_s.at[s, d], h_r.at[s, d], {"tp": t_peers[d]})
            for d in range(1, TP)
        ]

    order = [0] + far_first
    pass_on(0)
    loads[0].wait()
    loads[1].wait()
    for s in far_first:
        to_z[s].wait_recv()
        to_x[s] = send_x(s)
    expand(0)
    for k in range(1, Z + 1):
        if k < Z:
            pass_on(order[k])
        if k > 1:
            expand(order[k - 1])
    loads[2].wait()

    to_b, to_e = {}, {}
    half = wd.shape[0] // TP

    def contract_rows(s):
        for copy in to_h[s]:
            copy.wait_recv()
        total = None
        for j in range(TP):
            term = dot(hid[z_peers[s], j], wd[j * half : (j + 1) * half, :])
            total = term if total is None else total + term
        tags = x[z_peers[s], :, :, :, width:].reshape(rows, extra).astype(F32)
        at = lax.broadcasted_iota(jnp.int32, (rows, extra), 1)
        here = (at == ep) | (at == ep + experts)
        scale = jnp.sum(jnp.where(here, tags, 0.0), axis=-1, keepdims=True)
        y[s] = (total * scale).astype(BF16).reshape(C, X, seq, cols)
        to_b[s] = [
            send(
                y.at[s, c_peers[n // X], x_peers[n % X]], p.at[s, n], b_s.at[s, n], b_r.at[s, n],
                {"ep": ep_of(row, x_peers[n % X], c_peers[n // X])},
            )
            for n in list(range(1, C * X))[::-1]
        ]

    def join(s):
        total = y[s, core, col].astype(F32)
        for copy in to_b[s]:
            copy.wait_recv()
        for n in range(1, C * X):
            total = total + p[s, n].astype(F32)
        if s == 0:
            return total
        u[s] = total.astype(BF16)
        to_e[s] = send(
            u.at[s], v.at[s], e_s.at[s], e_r.at[s], {"ep": ep_of(z_peers[s], col, core)}
        )

    own = None
    for k in range(Z + 1):
        if k < Z:
            contract_rows(order[k])
        if k >= 1:
            done = join(order[k - 1])
            own = done if order[k - 1] == 0 else own
    result = own
    for s in range(1, Z):
        to_e[s].wait_recv()
        result = result + v[s].astype(F32)
    own_resid = resid[:, pl.ds(pl.multiple_of(tp * cols, cols), cols)]
    out[...] = (own_resid + result).astype(BF16)
    for copy in started:
        copy.wait_send()


def local(
    dims,
    tokens,
    old_state,
    query_weight,
    forget_weight,
    input_weight,
    lower_bound,
    head_gain,
    out_weight,
    mix_gain,
    ffn_gain,
    group_weight,
    expert_weight,
    routes,
    gate_weight,
    up_weight,
    down_weight,
):
    Z, C, X, TP = dims
    seq, width = tokens.shape
    heads, size = old_state.shape[1], old_state.shape[2]
    experts = expert_weight.shape[1]
    channels = query_weight.shape[1]
    hidden, cols = gate_weight.shape[2], down_weight.shape[2]
    vmem = pl.BlockSpec(memory_space=pltpu.VMEM)
    anywhere = pl.BlockSpec(memory_space=pl.ANY)
    chunks = 4 if seq % 4 == 0 else 1
    dma = pltpu.SemaphoreType.DMA
    new_state, part = pl.pallas_call(
        functools.partial(mix_kernel, chunks=chunks),
        out_shape=(
            jax.ShapeDtypeStruct(old_state.shape, F32),
            jax.ShapeDtypeStruct((seq, width), BF16),
        ),
        in_specs=[vmem] * 4 + [anywhere] * 5,
        out_specs=(anywhere, vmem),
        scratch_shapes=[
            pltpu.VMEM((width, channels), BF16),
            pltpu.VMEM((width, channels), BF16),
            pltpu.VMEM((width, channels), BF16),
            pltpu.VMEM((channels, width), BF16),
            pltpu.VMEM(old_state.shape, F32),
            pltpu.VMEM((heads, seq, size), F32),
            dma((4,)),
            dma((chunks,)),
            dma((chunks,)),
        ],
        name="mix",
    )(
        tokens, mix_gain[None], lower_bound[None], head_gain,
        query_weight, forget_weight, input_weight, out_weight, old_state,
    )
    extra = -(-2 * experts // 128) * 128
    block = (seq, width + extra)
    layer_out = pl.pallas_call(
        functools.partial(expert_kernel, dims),
        out_shape=jax.ShapeDtypeStruct((seq, cols), BF16),
        in_specs=[vmem] * 6 + [anywhere] * 3,
        out_specs=vmem,
        scratch_shapes=[
            pltpu.VMEM((width, hidden), BF16),
            pltpu.VMEM((width, hidden), BF16),
            pltpu.VMEM((hidden * TP, cols), BF16),
            pltpu.VMEM((TP, seq, width), BF16),
            pltpu.VMEM((seq, width), F32),
            pltpu.VMEM((Z, C, X) + block, BF16),
            pltpu.VMEM((Z, TP, C * X * seq, hidden), BF16),
            pltpu.VMEM((Z, C, X, seq, cols), BF16),
            pltpu.VMEM((Z, C * X, seq, cols), BF16),
            pltpu.VMEM((Z, seq, cols), BF16),
            pltpu.VMEM((Z, seq, cols), BF16),
            dma((3,)),
            dma((TP,)), dma((TP,)),
            dma((Z,)), dma((Z,)),
            dma((Z, X)), dma((Z, X)),
            dma((Z,)), dma((Z,)),
            dma((Z, TP)), dma((Z, TP)),
            dma((Z, C * X)), dma((Z, C * X)),
            dma((Z,)), dma((Z,)),
        ],
        compiler_params=pltpu.CompilerParams(collective_id=0, has_side_effects=True),
        name="experts",
    )(
        tokens, part, ffn_gain[None], group_weight.T, expert_weight.T, routes.T,
        gate_weight, up_weight, down_weight,
    )
    return (layer_out, new_state)


def solution(mesh):
    in_specs = (
        P("ep", None),
        P("ep", "tp", None, None),
        P(None, "tp"),
        P(None, "tp"),
        P(None, "tp"),
        P("tp"),
        P("tp", None),
        P("tp", None),
        P(),
        P(),
        P(),
        P(),
        P("ep", None),
        P("ep", None, "tp"),
        P("ep", None, "tp"),
        P("ep", None, "tp"),
    )
    out_specs = (P("ep", "tp"), P("ep", "tp", None, None))
    ep, tp = mesh.shape["ep"], mesh.shape["tp"]
    cores = 2
    across = tp
    dims = (ep // (cores * across), cores, across, tp)
    body = functools.partial(local, dims)
    return jax.shard_map(body, mesh=mesh, in_specs=in_specs, out_specs=out_specs, check_vma=False)
```
